256 devices in a mesh: sp: 32 (over z, x), fs: 4 (over y), tp: 2 (over core).
Axes of the slice: x: 4, y: 4, z: 8, core: 2. Of those that a mesh axis runs over, the one named last changes fastest.
Arguments:
- inputs: bfloat16 [4, 4096, 2048], P('fs', 'sp'), may hold values from -6 to 6
- input_norm_gain: bfloat16 [2048], replicated, may hold values from 0.099609375 to 1.8984375
- receptance_matrix: bfloat16 [2048, 1024], P('fs', 'tp'), may hold values from -0.125 to 0.125
- key_matrix: bfloat16 [2048, 1024], P('fs', 'tp'), may hold values from -0.125 to 0.125
- value_matrix: bfloat16 [2048, 1024], P('fs', 'tp'), may hold values from -0.125 to 0.125
- pooling_input_weight: bfloat16 [2048, 1024], P('fs', 'tp'), may hold values from -0.125 to 0.125
- decay_lower_matrix: bfloat16 [2048, 128], replicated, may hold values from -0.125 to 0.125
- decay_raise_matrix: bfloat16 [2, 64, 1024], P(None, None, 'tp'), may hold values from -1 to 1
- decay_offset_bias: float32 [2, 1024], P(None, 'tp'), may hold values from -13 to -3
- removal_lower_matrix: bfloat16 [2048, 128], replicated, may hold values from -0.125 to 0.125
- removal_raise_matrix: bfloat16 [2, 64, 1024], P(None, None, 'tp'), may hold values from -1 to 1
- removal_rate_bias: float32 [2, 1024], P(None, 'tp'), may hold values from -9 to 1.5
- tempo_scale: float32 [4, 2, 16, 4096], P('fs', None, 'tp', 'sp'), may hold values from 0.3 to 3.2, as said below
- sudden_decay_extra: float32 [4, 2, 16, 4096], P('fs', None, 'tp', 'sp'), may hold values from -2.8 to 0
- head_norm_gain: bfloat16 [1024], P('tp'), may hold values from 0.099609375 to 1.8984375
- group_mixing_weight: bfloat16 [4, 256, 256], P('tp'), may hold values from -0.375 to 0.375
- attention_output_matrix: bfloat16 [2048, 1024], P('fs', 'tp'), may hold values from -0.125 to 0.125
- pooling_output_matrix: bfloat16 [2048, 1024], P('fs', 'tp'), may hold values from -0.125 to 0.125
Outputs:
- mixed_out: bfloat16 [4, 4096, 2048], P('fs', ('sp', 'tp'))
The draws below stay inside these ranges and needn't reach their ends.
Inputs may be any that keep to these rules, and one draw needn't show every extreme that they name: `tempo_scale`: positive.
All inputs are finite; a program needn't handle non-finite values.
Results may differ from the reference program's by a relative error of at most 0.017.
Values may be sent and summed in bfloat16 or wider, within the bound.
No kernel may reach another device: no remote copies, remote signals or barrier semaphores. Data moves between devices by JAX's collectives and lax.ppermute only.
A program may use at most 128 MiB of HBM per device.

```python
import math
import jax
import jax.numpy as jnp
from jax import lax

D = 2048
HEADS_A = 16
HEAD = 64
DECAY_RANK = 64
RATE_RANK = 64
POOL_GROUPS = 4
GROUP_WIDTH = 256
T_DEV = 128
D_A = 1024
D_POOL = 1024
LEN = 4096
SEQS = 4
N_SP = 32


def slow_mask(key):
    marks = []
    for travel_direction in range(2):
        order = jax.random.permutation(jax.random.fold_in(key, 41 + travel_direction), HEADS_A)
        marks.append((order < HEADS_A // 2).astype(jnp.float32))
    return jnp.repeat(jnp.stack(marks, axis=0), HEAD, axis=1)


def draw_decay_offset_bias(key, part):
    slow = slow_mask(key)
    jitter = jax.random.uniform(jax.random.fold_in(key, 5), (2, HEADS_A * HEAD), jnp.float32, -0.5, 0.5)
    slow_level = jnp.log(1.0 / (6.0 * LEN)) + 0.1
    fast_level = math.log(1.0 / 60.0) + 0.5
    return slow * slow_level + (1.0 - slow) * fast_level + jitter


def draw_removal_rate_bias(key, part):
    slow = slow_mask(key)
    jitter = jax.random.uniform(jax.random.fold_in(key, 6), (2, HEADS_A * HEAD), jnp.float32, -0.5, 0.5)
    fast_vals = jax.random.uniform(jax.random.fold_in(key, 7), (2, HEADS_A * HEAD), jnp.float32, -1.5, 1.5)
    return slow * (jnp.log(8.0 / LEN) + jitter) + (1.0 - slow) * fast_vals


def draw_tempo_scale(key, part):
    low, high = (0.5, 2.0)
    factor = jnp.exp(jax.random.uniform(jax.random.fold_in(key, 21), (SEQS, 2, HEADS_A, N_SP), jnp.float32, math.log(low), math.log(high)))
    factor = jnp.repeat(factor, T_DEV, axis=3)
    jitter = jax.random.uniform(jax.random.fold_in(key, 22), (SEQS, 2, HEADS_A, LEN), jnp.float32, 0.8, 1.25)
    return factor * jitter


def draw_sudden_decay_extra(key, part):
    places = jax.random.randint(jax.random.fold_in(key, 31), (SEQS, 2, HEADS_A, 4), 0, LEN)
    kept = jax.random.uniform(jax.random.fold_in(key, 32), (SEQS, 2, HEADS_A, 4), jnp.float32, 0.5, 0.8)
    lost = jnp.log(kept)
    spots = jnp.arange(LEN)
    marked = jnp.where(spots[None, None, None, None, :] == places[..., None], lost[..., None], 0.0)
    return jnp.sum(marked, axis=3).astype(jnp.float32)


def levels(stream_key, shape, shards, smallest, high):
    def one(axis_at, blocks):
        heights = jax.random.uniform(jax.random.fold_in(jax.random.fold_in(stream_key, 6), axis_at), (blocks,), jnp.float32, smallest / len(shards), high / len(shards))
        return jnp.repeat(jnp.exp(heights), shape[axis_at] // blocks).reshape((-1,) + (1,) * (len(shape) - axis_at - 1))

    factor_of = one(*shards[0])
    for cut in shards[1:]:
        factor_of = factor_of * one(*cut)
    return factor_of


def scatter_about(key, shape, deviation, most, pieces=(), dtype=jnp.bfloat16):
    drawn = deviation * jax.random.normal(key, shape, jnp.float32)
    if pieces:
        drawn = drawn * levels(key, shape, pieces, -0.22, 0.18)
    return jnp.clip(drawn, -most, most).astype(dtype)


def setup_inputs(seed: int = 0) -> dict:
    keys = jax.random.split(jax.random.key(seed), 19)
    inputs = scatter_about(keys[0], (SEQS, LEN, D), 1.0, 6.0, ((0, 4), (1, 32)))
    input_norm_gain = jnp.clip(1.0 + 0.18 * jax.random.normal(keys[1], (D,), jnp.float32), 0.099609375, 1.8984375).astype(jnp.bfloat16)
    receptance_matrix = scatter_about(keys[2], (D, D_A), D ** -0.5, 0.125, ((0, 4), (1, 2)))
    key_matrix = scatter_about(keys[3], (D, D_A), D ** -0.5, 0.125, ((0, 4), (1, 2)))
    value_matrix = scatter_about(keys[4], (D, D_A), D ** -0.5, 0.125, ((0, 4), (1, 2)))
    pooling_input_weight = scatter_about(keys[5], (D, D_POOL), D ** -0.5, 0.125, ((0, 4), (1, 2)))
    decay_lower_matrix = scatter_about(keys[6], (D, 2 * DECAY_RANK), D ** -0.5, 0.125)
    decay_raise_matrix = scatter_about(keys[7], (2, DECAY_RANK, D_A), (DECAY_RANK // 2) ** -0.5, 1.0, ((2, 2),))
    decay_offset_bias = draw_decay_offset_bias(jax.random.fold_in(keys[18], 71), 0)
    removal_lower_matrix = scatter_about(keys[9], (D, 2 * RATE_RANK), D ** -0.5, 0.125)
    removal_raise_matrix = scatter_about(keys[10], (2, RATE_RANK, D_A), (RATE_RANK // 2) ** -0.5, 1.0, ((2, 2),))
    removal_rate_bias = draw_removal_rate_bias(jax.random.fold_in(keys[18], 71), 0)
    tempo_scale = draw_tempo_scale(jax.random.fold_in(keys[18], 71), 0)
    sudden_decay_extra = draw_sudden_decay_extra(jax.random.fold_in(keys[18], 71), 0)
    head_norm_gain = jnp.clip(1.0 + 0.18 * jax.random.normal(keys[14], (D_A,), jnp.float32), 0.099609375, 1.8984375).astype(jnp.bfloat16)
    group_mixing_weight = scatter_about(keys[15], (POOL_GROUPS, GROUP_WIDTH, GROUP_WIDTH), GROUP_WIDTH ** -0.5, 0.375, ((0, 2),))
    attention_output_matrix = scatter_about(keys[16], (D, D_A), (D_A + D_POOL) ** -0.5, 0.125, ((0, 4), (1, 2)))
    pooling_output_matrix = scatter_about(keys[17], (D, D_POOL), (D_A + D_POOL) ** -0.5, 0.125, ((0, 4), (1, 2)))
    return dict(inputs=inputs, input_norm_gain=input_norm_gain, receptance_matrix=receptance_matrix, key_matrix=key_matrix, value_matrix=value_matrix, pooling_input_weight=pooling_input_weight, decay_lower_matrix=decay_lower_matrix, decay_raise_matrix=decay_raise_matrix, decay_offset_bias=decay_offset_bias, removal_lower_matrix=removal_lower_matrix, removal_raise_matrix=removal_raise_matrix, removal_rate_bias=removal_rate_bias, tempo_scale=tempo_scale, sudden_decay_extra=sudden_decay_extra, head_norm_gain=head_norm_gain, group_mixing_weight=group_mixing_weight, attention_output_matrix=attention_output_matrix, pooling_output_matrix=pooling_output_matrix)


norm_eps = 1e-06
head_eps = 0.00064
unit_eps = 1e-06
highest = lax.Precision.HIGHEST

def project(left, weight):
    return jnp.dot(left, weight, preferred_element_type=jnp.float32).astype(jnp.bfloat16)

def window_diff(values, half):
    running = jnp.concatenate([jnp.zeros((1, values.shape[1]), jnp.float32), jnp.cumsum(values, axis=0)], axis=0)
    spots = jnp.arange(LEN)
    upper = jnp.minimum(spots + half, LEN)
    lower = jnp.maximum(spots - half, 0)
    counts = (upper - lower).astype(jnp.float32)
    return (running[upper] - running[lower]) / counts[:, None] - values

def recur(state, element_list):
    decay, unit, removal, written, value, recept = element_list
    pulled = jnp.einsum('hvk,hk->hv', state, unit, precision=highest)
    state = state * jnp.exp(decay)[:, None, :] - pulled[:, :, None] * removal[:, None, :] + value[:, :, None] * written[:, None, :]
    return (state, jnp.einsum('hvk,hk->hv', state, recept, precision=highest))

def reference(inputs, input_norm_gain, receptance_matrix, key_matrix, value_matrix, pooling_input_weight, decay_lower_matrix, decay_raise_matrix, decay_offset_bias, removal_lower_matrix, removal_raise_matrix, removal_rate_bias, tempo_scale, sudden_decay_extra, head_norm_gain, group_mixing_weight, attention_output_matrix, pooling_output_matrix):

    def single_sequence(element_list):
        row_block, decay_tempo, sudden_jump = element_list
        values = row_block.astype(jnp.float32)
        normed = (values * lax.rsqrt(lax.optimization_barrier(jnp.mean(values * values, axis=-1, keepdims=True)) + norm_eps) * input_norm_gain.astype(jnp.float32)).astype(jnp.bfloat16)
        receptance = project(normed, receptance_matrix).astype(jnp.float32).reshape(LEN, HEADS_A, HEAD)
        key_rows = project(normed, key_matrix).astype(jnp.float32).reshape(LEN, HEADS_A, HEAD)
        val_rows = project(normed, value_matrix).astype(jnp.float32).reshape(LEN, HEADS_A, HEAD)
        pool_in = project(normed, pooling_input_weight).astype(jnp.float32)
        decay_act = jnp.tanh(project(normed, decay_lower_matrix).astype(jnp.float32)).astype(jnp.bfloat16)
        rate_latent = project(normed, removal_lower_matrix)
        unit_keys = key_rows * lax.rsqrt(lax.optimization_barrier(jnp.sum(key_rows * key_rows, axis=-1, keepdims=True)) + unit_eps)
        readout = jnp.zeros((LEN, HEADS_A, HEAD), jnp.float32)
        for travel_direction in range(2):
            part = decay_act[:, travel_direction * DECAY_RANK:(travel_direction + 1) * DECAY_RANK]
            decay_pre = decay_offset_bias[travel_direction] + jnp.dot(part, decay_raise_matrix[travel_direction], preferred_element_type=jnp.float32)
            decay_velocity = jnp.exp(-jax.nn.softplus(-decay_pre) - 0.5).reshape(LEN, HEADS_A, HEAD)
            logarithm_decay = -decay_velocity * decay_tempo[travel_direction].T[:, :, None] + sudden_jump[travel_direction].T[:, :, None]
            latent = rate_latent[:, travel_direction * RATE_RANK:(travel_direction + 1) * RATE_RANK]
            rate = jax.nn.sigmoid(removal_rate_bias[travel_direction] + jnp.dot(latent, removal_raise_matrix[travel_direction], preferred_element_type=jnp.float32))
            rate = rate.reshape(LEN, HEADS_A, HEAD)
            start = jnp.zeros((HEADS_A, HEAD, HEAD), jnp.float32)
            _, reads = lax.scan(recur, start, (logarithm_decay, unit_keys, unit_keys * rate, key_rows * rate, val_rows, receptance), reverse=travel_direction == 1)
            readout = readout + reads
        centred = readout - lax.optimization_barrier(jnp.mean(readout, axis=-1, keepdims=True))
        spread = lax.optimization_barrier(jnp.mean(centred * centred, axis=-1, keepdims=True))
        attn_out = (centred * lax.rsqrt(spread + head_eps)).reshape(LEN, HEADS_A * HEAD) * head_norm_gain.astype(jnp.float32)
        attn_out = attn_out.astype(jnp.bfloat16)
        diffs = [window_diff(pool_in[:, group * GROUP_WIDTH:(group + 1) * GROUP_WIDTH], 2 ** group) for group in range(POOL_GROUPS)]
        pool_diff = jnp.concatenate(diffs, axis=1).astype(jnp.bfloat16)
        mixed = [jnp.dot(pool_diff[:, group * GROUP_WIDTH:(group + 1) * GROUP_WIDTH], group_mixing_weight[group], preferred_element_type=jnp.float32) for group in range(POOL_GROUPS)]
        pool_out = jnp.concatenate(mixed, axis=1).astype(jnp.bfloat16)
        merged = jnp.dot(attn_out, attention_output_matrix.T, preferred_element_type=jnp.float32) + jnp.dot(pool_out, pooling_output_matrix.T, preferred_element_type=jnp.float32)
        return merged.astype(jnp.bfloat16)
    return lax.map(single_sequence, (inputs, tempo_scale, sudden_decay_extra))
```

```python
import functools

import jax
import jax.numpy as jnp
from jax import lax
from jax.experimental import pallas as pl
from jax.experimental.pallas import tpu as pltpu
from jax.sharding import Mesh
from jax.sharding import PartitionSpec as P

SP = ("sp_0", "sp_1")
SP_TP = ("sp_0", "sp_1", "tp")
N_FS, N_X, N_Z = 4, 4, 8
TOK = 128
BLK = 32
N_BLK = TOK // BLK
PAIRS = 4
REACH = 8

norm_eps = 1e-06
head_eps = 0.00064
unit_eps = 1e-06
half_root = 0.6065306597126334
cap = 80.0

f32 = jnp.float32
bf16 = jnp.bfloat16
highest = lax.Precision.HIGHEST


def call(body, outs, scratch=(), flops=0, name=None):
    def run(scalars, *arrays):
        return pl.pallas_call(
            body,
            out_shape=[jax.ShapeDtypeStruct(s, d) for s, d in outs],
            in_specs=[pl.BlockSpec(memory_space=pltpu.SMEM)]
            + [pl.BlockSpec(memory_space=pltpu.VMEM)] * len(arrays),
            out_specs=[pl.BlockSpec(memory_space=pltpu.VMEM)] * len(outs),
            scratch_shapes=list(scratch),
            compiler_params=pltpu.CompilerParams(vmem_limit_bytes=48 << 20),
            cost_estimate=pl.CostEstimate(flops=flops, transcendentals=0, bytes_accessed=1 << 20),
            name=name,
        )(scalars, *arrays)

    return run


def dot(a, b):
    return jnp.dot(a, b, preferred_element_type=f32)


def dot_t(a, b):
    return lax.dot_general(a, b, (((1,), (1,)), ((), ())), preferred_element_type=f32)


def dot_0(a, b):
    return lax.dot_general(a, b, (((0,), (0,)), ((), ())), preferred_element_type=f32)


def iota2(shape):
    return (
        lax.broadcasted_iota(jnp.int32, shape, 0),
        lax.broadcasted_iota(jnp.int32, shape, 1),
    )


def roll64(a):
    return pltpu.roll(a, 64, axis=1)


def head_sum(a):
    row, lane = iota2((128, 128))
    same = jnp.where((row // 64) == (lane // 64), 1.0, 0.0).astype(f32)
    return jnp.dot(a, same, precision=highest, preferred_element_type=f32)


def mid_rows(way):
    return [i * BLK + (BLK // 2 - 1 if way == 0 else BLK // 2) for i in range(N_BLK)]


def both_heads(block, lane):
    zero = jnp.zeros_like(block)
    low = lane < 64
    return jnp.concatenate(
        [jnp.where(low, block, zero), jnp.where(low, zero, block)], axis=0
    ).astype(bf16)


def matmul_body(_, a0, a1, a2, a3, w1, w2, p0, p1, p2, p3):
    rows = jnp.concatenate([a0[...], a1[...], a2[...], a3[...]], axis=0)
    for half, w in enumerate((w1, w2)):
        got = dot(rows, w[...])
        cols = slice(half * 512, (half + 1) * 512)
        p0[:, cols] = got[:TOK]
        p1[:, cols] = got[TOK : 2 * TOK].astype(bf16)
        p2[:, cols] = got[2 * TOK : 3 * TOK].astype(bf16)
        p3[:, cols] = got[3 * TOK :].astype(bf16)


def maps_body(
    scal, own, r1, r2, r3, inv, act, lat, draise, dbias, rraise, rbias, tempo, sudden,
    o0, o1, o2, o3, right_out, reach_out, xy_out, maps,
):
    here = scal[0]
    row, lane = iota2((TOK, TOK))
    low = lane < 64
    wide_lane = lax.broadcasted_iota(jnp.int32, (TOK, 256), 1)
    wide_low = (wide_lane % 128) < 64
    eye = row == lane
    eye_bf = jnp.where(eye, 1.0, 0.0).astype(bf16)
    level_masks = []
    for level in range(7):
        size = 2**level
        hit = ((row // (2 * size)) == (lane // (2 * size))) & ((row // size) != (lane // size))
        level_masks.append(jnp.where(hit, 1.0, 0.0).astype(bf16))
    scale = inv[...]
    for pair in range(PAIRS):
        cols = slice(pair * 128, (pair + 1) * 128)
        vcols = slice(512 + pair * 128, 512 + (pair + 1) * 128)

        def total(c):
            got = own[:, c] + r1[:, c].astype(f32) + r2[:, c].astype(f32) + r3[:, c].astype(f32)
            return (got * scale).astype(bf16).astype(f32)

        key = total(cols)
        val = total(vcols)
        square = head_sum(key * key) + unit_eps
        inverse = lax.rsqrt(square)
        unit = key * inverse
        strong = val * (square * inverse)
        links = []
        sides = []
        tails = []
        ends = []
        for way in range(2):
            mine = (lane // 64) == way
            pre = dbias[way : way + 1, cols] + dot(
                jnp.where(mine, act[...], jnp.zeros_like(act[...])), draise[:, cols]
            )
            rate = jax.nn.sigmoid(
                rbias[way : way + 1, cols]
                + dot(jnp.where(mine, lat[...], jnp.zeros_like(lat[...])), rraise[:, cols])
            )
            at = way * 8 + pair * 2
            pace = jnp.where(low, tempo[:, at : at + 1], tempo[:, at + 1 : at + 2])
            jump = jnp.where(low, sudden[:, at : at + 1], sudden[:, at + 1 : at + 2])
            g = -half_root * jax.nn.sigmoid(pre) * pace + jump
            tri = (row >= lane) if way == 0 else (row <= lane)
            reach = jnp.dot(
                jnp.where(tri, 1.0, 0.0).astype(f32), g, precision=highest, preferred_element_type=f32
            )
            reach_out[way, :, cols] = reach
            removal = unit * rate
            before = reach - g
            pieces = []
            for i, mid_row in enumerate(mid_rows(way)):
                mid = reach[mid_row : mid_row + 1, :]
                rows = slice(i * BLK, (i + 1) * BLK)
                left = unit[rows] * jnp.exp(before[rows] - mid)
                right = (removal * jnp.exp(jnp.minimum(mid - reach, cap))).astype(bf16)
                right_out[way * PAIRS + pair, i] = right
                pieces.append(dot_t(both_heads(left, lane[:BLK]), right))
            strict = (row > lane) if way == 0 else (row < lane)
            for head in range(2):
                link = jnp.concatenate(
                    [piece[head * BLK : (head + 1) * BLK] for piece in pieces], axis=0
                )
                links.append(jnp.where(strict, link, 0.0).astype(bf16))
            sides.append(
                jnp.concatenate([strong, unit * jnp.exp(before)], axis=1).astype(bf16)
            )
            end = reach[TOK - 1 :, :] if way == 0 else reach[:1, :]
            tails.append((removal * jnp.exp(end - reach)).astype(bf16))
            ends.append(end)
        solved = [eye_bf - link * level_masks[0] for link in links]
        for level in range(1, 7):
            inner = [
                dot(link * level_masks[level], t).astype(bf16) for link, t in zip(links, solved)
            ]
            solved = [t - dot(t, part).astype(bf16) for t, part in zip(solved, inner)]
        for way in range(2):
            first = dot(solved[2 * way], sides[way])
            second = dot(solved[2 * way + 1], sides[way])
            xy = jnp.where(wide_low, first, second).astype(bf16)
            xy_out[way * PAIRS + pair] = xy
            got = dot_0(tails[way], xy)
            carry = got[:, :128]
            turn = jnp.where(eye, jnp.exp(ends[way]) - 1.0, 0.0) - got[:, 128:]
            packed = jnp.where(
                row < 64,
                jnp.where(low, carry, roll64(turn)),
                jnp.where(low, roll64(carry), turn),
            )
            maps[pair, way] = packed.astype(bf16)
    for s, out in enumerate((o0, o1, o2, o3)):
        out[...] = maps[(here + s) & 3]


def read_body(_, own, r1, r2, r3, inv, right, reach_in, xy_in, qeff, local):
    row, lane = iota2((TOK, TOK))
    wide_low = (lax.broadcasted_iota(jnp.int32, (TOK, 256), 1) % 128) < 64
    scale = inv[...]
    for pair in range(PAIRS):
        c = slice(pair * 128, (pair + 1) * 128)
        got = own[:, c] + r1[:, c].astype(f32) + r2[:, c].astype(f32) + r3[:, c].astype(f32)
        query = (got * scale).astype(bf16).astype(f32)
        base = None
        for way in range(2):
            reach = reach_in[way, :, c]
            pieces = []
            for i, mid_row in enumerate(mid_rows(way)):
                mid = reach[mid_row : mid_row + 1, :]
                rows = slice(i * BLK, (i + 1) * BLK)
                left = query[rows] * jnp.exp(reach[rows] - mid)
                pieces.append(
                    dot_t(both_heads(left, lane[:BLK]), right[way * PAIRS + pair, i])
                )
            within = (row >= lane) if way == 0 else (row <= lane)
            xy = xy_in[way * PAIRS + pair]
            pulls = []
            for head in range(2):
                link = jnp.concatenate(
                    [piece[head * BLK : (head + 1) * BLK] for piece in pieces], axis=0
                )
                pulls.append(dot(jnp.where(within, link, 0.0).astype(bf16), xy))
            pull = jnp.where(wide_low, pulls[0], pulls[1])
            base = pull[:, :128] if base is None else base + pull[:, :128]
            qeff[pair, :, way * 128 : (way + 1) * 128] = (
                query * jnp.exp(reach) - pull[:, 128:]
            ).astype(bf16)
        local[:, c] = base


def spread(packed, row, lane):
    moved = roll64(packed)
    return jnp.where(
        row < 64,
        jnp.where(lane < 64, moved, 0.0),
        jnp.where(lane < 64, 0.0, packed),
    ).astype(bf16)


def chain_body(scal, a0, a1, a2, a3, *rest):
    sends, before, maps = rest[:7], rest[7], rest[8]
    here, level = scal[0], scal[1]
    row, lane = iota2((TOK, TOK))
    ident = jnp.where((lane - 64) == (row % 64), 1.0, 0.0).astype(f32)
    for s, a in enumerate((a0, a1, a2, a3)):
        maps[s] = a[...]
    totals = []
    for way in range(2):
        state = None
        for step in range(N_X):
            at = step if way == 0 else N_X - 1 - step
            got = maps[(here - at) & 3, way].astype(f32)
            if state is None:
                state = got + ident
            else:
                state = (
                    state
                    + dot(spread(got, row, lane), state.astype(bf16))
                    + jnp.where(lane < 64, got, 0.0)
                )
            if step < N_X - 1:
                before[step, way] = (state - ident).astype(bf16)
        totals.append((state - ident))
    for s, send in enumerate(sends, start=1):
        send[...] = jnp.where(level + s < N_Z, totals[0], totals[1]).astype(bf16)


def apply_body(scal, *refs):
    got, before, outs, states = refs[:7], refs[7], refs[8:12], refs[12]
    here, level = scal[0], scal[1]
    row, lane = iota2((TOK, TOK))

    def step(state, packed):
        packed = packed.astype(f32)
        fresh = jnp.where(lane < 64, packed, 0.0)
        if state is None:
            return fresh
        return state + dot(spread(packed, row, lane), state.astype(bf16)) + fresh

    enter = []
    for way in range(2):
        state = jnp.zeros((TOK, TOK), f32)
        for k in range(1, N_Z):
            s = N_Z - k if way == 0 else k
            used = (s <= level) if way == 0 else (s > level)
            state = step(state, jnp.where(used, got[s - 1][...].astype(f32), 0.0))
        enter.append(state)
    for at in range(N_X):
        f = enter[0] if at == 0 else step(enter[0], before[at - 1, 0])
        back = N_X - 1 - at
        b = enter[1] if back == 0 else step(enter[1], before[back - 1, 1])
        states[at] = jnp.where(lane < 64, f, roll64(b)).astype(bf16)
    for s, out in enumerate(outs):
        out[...] = states[(here + s) & 3]


def final_body(
    scal, z0, z1, z2, z3, qeff, local, hgain, w0, w1, w2, w3, pool, keep, give, states, total
):
    here, seq, core = scal[0], scal[2], scal[3]
    row, lane = iota2((TOK, TOK))
    low = lane < 64
    top = row < 64
    for s, z in enumerate((z0, z1, z2, z3)):
        states[s] = z[...]
    cols = []
    for pair in range(PAIRS):
        c = slice(pair * 128, (pair + 1) * 128)
        packed = states[(here - pair) & 3].astype(f32)
        moved = roll64(packed)
        ahead = jnp.where(top, jnp.where(low, packed, 0.0), jnp.where(low, 0.0, moved))
        behind = jnp.where(top, jnp.where(low, moved, 0.0), jnp.where(low, 0.0, packed))
        block = jnp.concatenate([ahead, behind], axis=0).astype(bf16)
        read = dot(qeff[pair], block) + local[:, c]
        centred = read - head_sum(read) * (1.0 / 64.0)
        var = head_sum(centred * centred) * (1.0 / 64.0)
        cols.append(
            (centred * lax.rsqrt(var + head_eps) * hgain[:, c].astype(f32)).astype(bf16)
        )
    attn = jnp.concatenate(cols, axis=1)
    for s, w in enumerate((w0, w1, w2, w3)):
        at = pl.multiple_of(((seq - s) & 3) * 512, 512)
        total[:, pl.ds(at, 512)] = dot_t(attn, w[...]) + pool[:, pl.ds(at, 512)]
    mine = pl.multiple_of(core * 64, 64)
    other = pl.multiple_of((1 - core) * 64, 64)
    keep[...] = total[pl.ds(mine, 64), :]
    give[...] = total[pl.ds(other, 64), :].astype(bf16)


def pool_body(scal, pool_in, head, tail, mix, w0, w1, w2, w3, out):
    seq, core, span = scal[2], scal[3], scal[4]
    here = pool_in[...].astype(f32)
    cells = jnp.concatenate([tail[...].astype(f32), here, head[...].astype(f32)], axis=0)
    spot = lax.broadcasted_iota(jnp.int32, (TOK, 256), 0) + span * TOK
    length = TOK * N_X * N_Z
    sums = []
    running = cells
    for level in range(4):
        shift = 2**level
        size = running.shape[0]
        running = running[: size - shift] + running[shift:]
        sums.append(running[REACH - shift : REACH - shift + TOK])
    mixed = []
    for member in range(2):
        c = slice(member * 256, (member + 1) * 256)
        upper = core == 1
        chosen = jnp.where(upper, sums[member + 2][:, c], sums[member][:, c])
        half = jnp.where(upper, 2 ** (member + 2), 2**member)
        count = (jnp.minimum(spot + half, length) - jnp.maximum(spot - half, 0)).astype(f32)
        diff = (chosen / count - here[:, c]).astype(bf16)
        mixed.append(dot(diff, mix[member]).astype(bf16))
    pooled = jnp.concatenate(mixed, axis=1)
    for s, w in enumerate((w0, w1, w2, w3)):
        at = pl.multiple_of(((seq - s) & 3) * 512, 512)
        out[:, pl.ds(at, 512)] = dot_t(pooled, w[...])


def shift_by(a, axis, s, n):
    return lax.ppermute(a, axis, [(i, (i + s) % n) for i in range(n)])


def shards(
    inputs,
    input_norm_gain,
    receptance_matrix,
    key_matrix,
    value_matrix,
    pooling_input_weight,
    decay_lower_matrix,
    decay_raise_matrix,
    decay_offset_bias,
    removal_lower_matrix,
    removal_raise_matrix,
    removal_rate_bias,
    tempo_scale,
    sudden_decay_extra,
    head_norm_gain,
    group_mixing_weight,
    attention_output_matrix,
    pooling_output_matrix,
):
    seq = lax.axis_index("fs")
    core = lax.axis_index("tp")
    level = lax.axis_index("sp_0")
    here = lax.axis_index("sp_1")
    span = level * N_X + here
    scal = jnp.stack([here, level, seq, core, span]).astype(jnp.int32)
    tokens = inputs[0]
    wide = tokens.astype(f32)
    gained = (wide * input_norm_gain.astype(f32)).astype(bf16)

    def block(s):
        return lax.dynamic_slice(gained, (0, ((seq + s) % N_FS) * 512), (TOK, 512))

    rows = [block(0)] + [None] * 3
    for s in (2, 1, 3):
        rows[s] = shift_by(block(s), "fs", s, N_FS)
    inv = lax.rsqrt(jnp.mean(wide * wide, axis=-1, keepdims=True) + norm_eps)
    act = jnp.tanh((dot(gained, decay_lower_matrix) * inv).astype(bf16).astype(f32)).astype(bf16)
    lat = (dot(gained, removal_lower_matrix) * inv).astype(bf16)
    tempo = tempo_scale[0].reshape(16, TOK).T
    sudden = sudden_decay_extra[0].reshape(16, TOK).T

    part_shapes = [((TOK, 1024), f32)] + [((TOK, 1024), bf16)] * 3

    def partials(first, second, name):
        got = call(matmul_body, part_shapes, flops=1 << 29, name=name)(scal, *rows, first, second)
        back = [None] * 4
        back[0] = got[0]
        for s in (2, 1, 3):
            back[s] = shift_by(got[s], "fs", N_FS - s, N_FS)
        return back

    kv = partials(key_matrix, value_matrix, "project_kv")
    qp = partials(receptance_matrix, pooling_input_weight, "project_qp")

    outs = call(
        maps_body,
        [((2, TOK, TOK), bf16)] * 4
        + [((8, N_BLK, TOK, TOK), bf16), ((2, TOK, 512), f32), ((8, TOK, 256), bf16)],
        scratch=[pltpu.VMEM((PAIRS, 2, TOK, TOK), bf16)],
        flops=1 << 33,
        name="maps",
    )(
        scal, *kv, inv, act, lat,
        decay_raise_matrix.reshape(128, 512), decay_offset_bias,
        removal_raise_matrix.reshape(128, 512), removal_rate_bias,
        tempo, sudden,
    )
    maps, (right, reach, xy) = outs[:4], outs[4:]
    got = [maps[0]] + [shift_by(maps[s], "sp_1", s, N_X) for s in (1, 2, 3)]

    attn_own, pool_own, _ = lax.optimization_barrier(
        (attention_output_matrix, pooling_output_matrix, kv[1])
    )
    attn_w = [attn_own] + [shift_by(attn_own, "fs", s, N_FS) for s in (1, 2, 3)]
    pool_w = [pool_own] + [shift_by(pool_own, "fs", s, N_FS) for s in (1, 2, 3)]

    pool_sum = qp[0][:, 512:]
    for s in (1, 2, 3):
        pool_sum = pool_sum + qp[s][:, 512:].astype(f32)
    pool_in = (pool_sum * inv).astype(bf16)
    n_sp = N_X * N_Z
    tail = lax.ppermute(pool_in[TOK - REACH :], SP, [(i, i + 1) for i in range(n_sp - 1)])
    head = lax.ppermute(pool_in[:REACH], SP, [(i + 1, i) for i in range(n_sp - 1)])

    qeff, local = call(
        read_body,
        [((PAIRS, TOK, 256), bf16), ((TOK, 512), f32)],
        flops=1 << 31,
        name="reads",
    )(scal, *qp, inv, right, reach, xy)

    outs = call(
        chain_body,
        [((TOK, TOK), bf16)] * 7 + [((3, 2, TOK, TOK), bf16)],
        scratch=[pltpu.VMEM((N_X, 2, TOK, TOK), bf16)],
        flops=1 << 29,
        name="chain",
    )(scal, *got)
    sends, before = outs[:7], outs[7]
    passed = [shift_by(sends[s - 1], "sp_0", s, N_Z) for s in range(1, N_Z)]

    (pool_part,) = call(pool_body, [((TOK, 2048), f32)], flops=1 << 30, name="pool")(
        scal, pool_in, head, tail, group_mixing_weight, *pool_w
    )

    states = call(
        apply_body,
        [((TOK, TOK), bf16)] * 4,
        scratch=[pltpu.VMEM((N_X, TOK, TOK), bf16)],
        flops=1 << 29,
        name="enter",
    )(scal, *passed, before)
    enter = [states[0]] + [shift_by(states[s], "sp_1", s, N_X) for s in (1, 2, 3)]

    keep, give = call(
        final_body,
        [((64, 2048), f32), ((64, 2048), bf16)],
        scratch=[pltpu.VMEM((N_X, TOK, TOK), bf16), pltpu.VMEM((TOK, 2048), f32)],
        flops=1 << 30,
        name="final",
    )(scal, *enter, qeff, local, head_norm_gain.reshape(1, 512), *attn_w, pool_part)
    taken = lax.ppermute(give, "tp", [(0, 1), (1, 0)])
    return (keep + taken.astype(f32)).astype(bf16)[None]


def solution(mesh):
    split = Mesh(
        mesh.devices.reshape(8, 4, mesh.shape["fs"], mesh.shape["tp"]), ("sp_0", "sp_1", "fs", "tp")
    )
    in_specs = (
        P("fs", SP, None),
        P(),
        P("fs", "tp"),
        P("fs", "tp"),
        P("fs", "tp"),
        P("fs", "tp"),
        P(),
        P(None, None, "tp"),
        P(None, "tp"),
        P(),
        P(None, None, "tp"),
        P(None, "tp"),
        P("fs", None, "tp", SP),
        P("fs", None, "tp", SP),
        P("tp"),
        P("tp", None, None),
        P("fs", "tp"),
        P("fs", "tp"),
    )
    out_specs = P("fs", SP_TP, None)
    return jax.shard_map(
        shards, mesh=split, in_specs=in_specs, out_specs=out_specs, check_vma=False
    )
```

```python
import jax
import jax.numpy as jnp
from jax import lax
from jax.experimental import pallas as pl
from jax.experimental.pallas import tpu as pltpu
from jax.sharding import Mesh
from jax.sharding import PartitionSpec as P

SP = ("sp_0", "sp_1")
SP_TP = ("sp_0", "sp_1", "tp")
N_FS, N_X, N_Z = 4, 4, 8
TOK = 128
BLK = 32
N_BLK = TOK // BLK
PAIRS = 4
REACH = 8
LEFT, LEAD, TAIL, OWN = 4, 5, 6, 7

norm_eps = 1e-06
head_eps = 0.00064
unit_eps = 1e-06
half_root = 0.6065306597126334
cap = 80.0

f32 = jnp.float32
bf16 = jnp.bfloat16
highest = lax.Precision.HIGHEST


def in_hbm(array):
    return pltpu.with_memory_space_constraint(array, pltpu.HBM)


def call(body, outs, scratch=(), far=0, same=None):
    def run(scal, *arrays):
        count = len(arrays) - far + len(outs)

        def fetched(at, *refs):
            source, near, held = refs[:far], refs[far : far + count], refs[far + count :]
            buffers, sems, rest = held[:far], held[far], held[far + 1 :]
            copies = [
                pltpu.make_async_copy(a, b, sems.at[k])
                for k, (a, b) in enumerate(zip(source, buffers))
            ]
            for copy in copies:
                copy.start()
            for copy in copies:
                copy.wait()
            body(at, *buffers, *near, *rest)

        extra = []
        if far:
            extra = [pltpu.VMEM(a.shape, a.dtype) for a in arrays[:far]]
            extra.append(pltpu.SemaphoreType.DMA((far,)))
        return pl.pallas_call(
            fetched if far else body,
            out_shape=[jax.ShapeDtypeStruct(s, d) for s, d in outs],
            in_specs=[pl.BlockSpec(memory_space=pltpu.SMEM)]
            + [pl.BlockSpec(memory_space=pltpu.HBM)] * far
            + [pl.BlockSpec(memory_space=pltpu.VMEM)] * (len(arrays) - far),
            out_specs=[pl.BlockSpec(memory_space=pltpu.VMEM)] * len(outs),
            scratch_shapes=extra + list(scratch),
            input_output_aliases=same or {},
            compiler_params=pltpu.CompilerParams(vmem_limit_bytes=20 << 20),
            cost_estimate=pl.CostEstimate(flops=1, transcendentals=0, bytes_accessed=1),
        )(scal, *[in_hbm(a) for a in arrays[:far]], *arrays[far:])

    return run


def seat(scal, axis):
    return scal[("sp_1", "sp_0", "fs", "tp").index(axis)]


def stage_body(scal, *refs):
    count = len(refs) // 2
    sems = refs[-1]
    copies = [pltpu.make_async_copy(refs[k], refs[count + k], sems.at[k]) for k in range(count)]
    for copy in copies:
        copy.start()
    for copy in copies:
        copy.wait()


def stage(scal, *arrays):
    return pl.pallas_call(
        stage_body,
        out_shape=[jax.ShapeDtypeStruct(a.shape, a.dtype) for a in arrays],
        in_specs=[pl.BlockSpec(memory_space=pltpu.SMEM)]
        + [pl.BlockSpec(memory_space=pltpu.HBM)] * len(arrays),
        out_specs=[pl.BlockSpec(memory_space=pltpu.VMEM)] * len(arrays),
        scratch_shapes=[pltpu.SemaphoreType.DMA((len(arrays),))],
        compiler_params=pltpu.CompilerParams(vmem_limit_bytes=4 << 20),
        name="stage",
    )(scal, *[in_hbm(a) for a in arrays])


def cut_body(scal, tokens, *refs):
    outs, sems = refs[:4], refs[4]
    copies = []
    for s, out in enumerate(outs):
        at = pl.multiple_of(((seat(scal, "fs") + s) & 3) * 512, 512)
        copies.append(pltpu.make_async_copy(tokens.at[:, pl.ds(at, 512)], out, sems.at[s]))
        copies[-1].start()
    for copy in copies:
        copy.wait()


def dot(a, b):
    return jnp.dot(a, b, preferred_element_type=f32)


def dot_t(a, b):
    return lax.dot_general(a, b, (((1,), (1,)), ((), ())), preferred_element_type=f32)


def dot_0(a, b):
    return lax.dot_general(a, b, (((0,), (0,)), ((), ())), preferred_element_type=f32)


def iota2(shape):
    return (
        lax.broadcasted_iota(jnp.int32, shape, 0),
        lax.broadcasted_iota(jnp.int32, shape, 1),
    )


def roll64(a):
    return pltpu.roll(a, 64, axis=1)


def summed(own, parts, cols, scale):
    r1, r2, r3 = parts
    got = own + r1[:, cols].astype(f32)
    got = got + r2[:, cols].astype(f32) + r3[:, cols].astype(f32)
    return (got * scale).astype(bf16).astype(f32)


def head_sum(a):
    row, lane = iota2((128, 128))
    same = jnp.where((row // 64) == (lane // 64), 1.0, 0.0).astype(f32)
    return jnp.dot(a, same, precision=highest, preferred_element_type=f32)


def mid_rows(way):
    return [i * BLK + (BLK // 2 - 1 if way == 0 else BLK // 2) for i in range(N_BLK)]


def both_heads(block, lane):
    zero = jnp.zeros_like(block)
    low = lane < 64
    return jnp.concatenate(
        [jnp.where(low, block, zero), jnp.where(low, zero, block)], axis=0
    ).astype(bf16)


def gather_rows(scal, gain, parts):
    at = pl.multiple_of(seat(scal, "fs") * 512, 512)
    rows = jnp.concatenate([part[...] for part in parts], axis=0).astype(f32)
    return (rows * gain[:, pl.ds(at, 512)].astype(f32)).astype(bf16)


def put_parts(got, outs, cols):
    for s in (1, 2, 3):
        outs[s - 1][:, cols] = got[s * TOK : (s + 1) * TOK].astype(bf16)


def project_qp_body(scal, gain, w1, w2, a0, a1, a2, a3, own, *outs):
    rows = gather_rows(scal, gain, (a0, a1, a2, a3))
    for half, w in enumerate((w1, w2)):
        cols = slice(half * 512, (half + 1) * 512)
        got = dot(rows, w[...])
        own[:, cols] = got[:TOK]
        put_parts(got, outs, cols)


def project_kv_body(scal, gain, w1, w2, a0, a1, a2, a3, *outs):
    rows = gather_rows(scal, gain, (a0, a1, a2, a3))
    for half, w in enumerate((w1, w2)):
        put_parts(dot(rows, w[...]), outs, slice(half * 512, (half + 1) * 512))


def decay_body(
    scal,
    tokens, gain, dlow, rlow, draise, dbias, rraise, rbias, tempo_in, sudden_in, wk, wv, mine,
    inv_out, reach_out, out,
):
    rows = gather_rows(scal, gain, (mine,))
    for half, w in enumerate((wk, wv)):
        got = dot(rows, w[...])
        for pair in range(PAIRS):
            out[half * PAIRS + pair, OWN] = got[:, pair * 128 : (pair + 1) * 128].astype(bf16)
    row, lane = iota2((TOK, TOK))
    low = lane < 64
    tempo = tempo_in[...].T
    sudden = sudden_in[...].T
    wide = tokens[...].astype(f32)
    inv = lax.rsqrt(jnp.mean(wide * wide, axis=-1, keepdims=True) + norm_eps)
    inv_out[...] = inv
    normed = (wide * inv * gain[...].astype(f32)).astype(bf16)
    act = jnp.tanh(dot(normed, dlow[...]).astype(bf16).astype(f32)).astype(bf16)
    lat = dot(normed, rlow[...]).astype(bf16)
    for way in range(2):
        mine = (lane // 64) == way
        act_w = jnp.where(mine, act, jnp.zeros_like(act))
        lat_w = jnp.where(mine, lat, jnp.zeros_like(lat))
        tri = jnp.where((row >= lane) if way == 0 else (row <= lane), 1.0, 0.0).astype(f32)
        for pair in range(PAIRS):
            cols = slice(pair * 128, (pair + 1) * 128)
            chain = way * PAIRS + pair
            pre = dbias[way : way + 1, cols] + dot(act_w, draise[:, cols])
            rate = jax.nn.sigmoid(rbias[way : way + 1, cols] + dot(lat_w, rraise[:, cols]))
            at = way * 8 + pair * 2
            pace = jnp.where(low, tempo[:, at : at + 1], tempo[:, at + 1 : at + 2])
            jump = jnp.where(low, sudden[:, at : at + 1], sudden[:, at + 1 : at + 2])
            g = -half_root * jax.nn.sigmoid(pre) * pace + jump
            reach = jnp.dot(tri, g, precision=highest, preferred_element_type=f32)
            reach_out[way, :, cols] = reach
            before = reach - g
            out[chain, LEAD] = jnp.exp(before).astype(bf16)
            for i, mid_row in enumerate(mid_rows(way)):
                mid = reach[mid_row : mid_row + 1, :]
                rows = slice(i * BLK, (i + 1) * BLK)
                out[chain, LEFT, rows] = jnp.exp(before[rows] - mid).astype(bf16)
                out[chain, i] = (rate * jnp.exp(jnp.minimum(mid - reach, cap))).astype(bf16)
            end = reach[TOK - 1 :, :] if way == 0 else reach[:1, :]
            out[chain, TAIL] = (rate * jnp.exp(end - reach)).astype(bf16)


def maps_body(
    scal,
    r1, r2, r3, inv, factors, reach,
    o0, o1, o2, o3, right_out, xy_out, solved, links, inner, ahead_out, tail_out, strong_out, maps,
):
    here = seat(scal, "sp_1")
    row, lane = iota2((TOK, TOK))
    low = lane < 64
    wide_low = (lax.broadcasted_iota(jnp.int32, (TOK, 256), 1) % 128) < 64
    eye = row == lane
    eye_bf = jnp.where(row == lane, 1.0, 0.0).astype(bf16)
    level_masks = []
    for level in range(7):
        size = 2**level
        hit = ((row // (2 * size)) == (lane // (2 * size))) & ((row // size) != (lane // size))
        level_masks.append(jnp.where(hit, 1.0, 0.0).astype(bf16))
    scale = inv[...]
    for pair in range(PAIRS):
        c = slice(pair * 128, (pair + 1) * 128)
        v = slice(512 + pair * 128, 512 + (pair + 1) * 128)
        key = summed(factors[pair, OWN].astype(f32), (r1, r2, r3), c, scale)
        square = head_sum(key * key) + unit_eps
        inverse = lax.rsqrt(square)
        unit = key * inverse
        val = summed(factors[PAIRS + pair, OWN].astype(f32), (r1, r2, r3), v, scale)
        strong_out[pair] = (val * (square * inverse)).astype(bf16)
        for way in range(2):
            chain = way * PAIRS + pair
            pieces = []
            for i in range(N_BLK):
                rows = slice(i * BLK, (i + 1) * BLK)
                side = (unit * factors[chain, i].astype(f32)).astype(bf16)
                right_out[chain, i] = side
                pieces.append(
                    dot_t(both_heads(unit[rows] * factors[chain, LEFT, rows].astype(f32), lane[:BLK]), side)
                )
            strict = (row > lane) if way == 0 else (row < lane)
            for head in range(2):
                link = jnp.concatenate(
                    [piece[head * BLK : (head + 1) * BLK] for piece in pieces], axis=0
                )
                link = jnp.where(strict, link, 0.0).astype(bf16)
                links[2 * chain + head] = link
                solved[2 * chain + head] = eye_bf - link * level_masks[0]
            ahead_out[chain] = (unit * factors[chain, LEAD].astype(f32)).astype(bf16)
            tail_out[chain] = (unit * factors[chain, TAIL].astype(f32)).astype(bf16)
    for level in range(1, 7):
        for k in range(16):
            inner[k] = dot(links[k] * level_masks[level], solved[k]).astype(bf16)
        for k in range(16):
            solved[k] = solved[k] - dot(solved[k], inner[k]).astype(bf16)
    for pair in range(PAIRS):
        c = slice(pair * 128, (pair + 1) * 128)
        for way in range(2):
            chain = way * PAIRS + pair
            side = jnp.concatenate([strong_out[pair], ahead_out[chain]], axis=1)
            first = dot(solved[2 * chain], side)
            second = dot(solved[2 * chain + 1], side)
            xy = jnp.where(wide_low, first, second).astype(bf16)
            xy_out[chain] = xy
            got = dot_0(tail_out[chain], xy)
            carry = got[:, :128]
            end = reach[way, TOK - 1 :, c] if way == 0 else reach[way, :1, c]
            turn = jnp.where(eye, jnp.exp(end) - 1.0, 0.0) - got[:, 128:]
            maps[pair, way] = jnp.where(
                row < 64,
                jnp.where(low, carry, roll64(turn)),
                jnp.where(low, roll64(carry), turn),
            ).astype(bf16)
    for s, out in enumerate((o0, o1, o2, o3)):
        out[...] = maps[(here + s) & 3]


def read_body(scal, own, r1, r2, r3, inv, right, reach_in, xy_in, qeff, local):
    row, lane = iota2((TOK, TOK))
    wide_low = (lax.broadcasted_iota(jnp.int32, (TOK, 256), 1) % 128) < 64
    scale = inv[...]
    for pair in range(PAIRS):
        c = slice(pair * 128, (pair + 1) * 128)
        query = summed(own[:, c], (r1, r2, r3), c, scale)
        base = None
        for way in range(2):
            reach = reach_in[way, :, c]
            pieces = []
            for i, mid_row in enumerate(mid_rows(way)):
                mid = reach[mid_row : mid_row + 1, :]
                rows = slice(i * BLK, (i + 1) * BLK)
                left = query[rows] * jnp.exp(reach[rows] - mid)
                pieces.append(
                    dot_t(both_heads(left, lane[:BLK]), right[way * PAIRS + pair, i])
                )
            within = (row >= lane) if way == 0 else (row <= lane)
            xy = xy_in[way * PAIRS + pair]
            pulls = []
            for head in range(2):
                link = jnp.concatenate(
                    [piece[head * BLK : (head + 1) * BLK] for piece in pieces], axis=0
                )
                pulls.append(dot(jnp.where(within, link, 0.0).astype(bf16), xy))
            pull = jnp.where(wide_low, pulls[0], pulls[1])
            base = pull[:, :128] if base is None else base + pull[:, :128]
            qeff[pair, :, way * 128 : (way + 1) * 128] = (
                query * jnp.exp(reach) - pull[:, 128:]
            ).astype(bf16)
        local[:, c] = base


def spread(packed, row, lane):
    moved = roll64(packed)
    return jnp.where(
        row < 64,
        jnp.where(lane < 64, moved, 0.0),
        jnp.where(lane < 64, 0.0, packed),
    ).astype(bf16)


def compose(state, packed, row, lane):
    return (
        state
        + dot(spread(packed, row, lane), state.astype(bf16))
        + jnp.where(lane < 64, packed, 0.0)
    )


def chain_body(scal, a0, a1, a2, a3, send, before, maps):
    here = seat(scal, "sp_1")
    row, lane = iota2((TOK, TOK))
    ident = jnp.where((lane - 64) == (row % 64), 1.0, 0.0).astype(f32)
    for s, a in enumerate((a0, a1, a2, a3)):
        maps[s] = a[...]
    for way in range(2):
        state = ident
        for step in range(N_X):
            at = step if way == 0 else N_X - 1 - step
            got = maps[(here - at) & 3, way].astype(f32)
            state = got + ident if step == 0 else compose(state, got, row, lane)
            if step < N_X - 1:
                before[step, way] = (state - ident).astype(bf16)
        send[way] = (state - ident).astype(bf16)


def group_body(scal, a0, a1, a2, a3, send, mine, maps):
    level = seat(scal, "sp_0")
    spot = level & 3
    row, lane = iota2((TOK, TOK))
    ident = jnp.where((lane - 64) == (row % 64), 1.0, 0.0).astype(f32)
    for s, a in enumerate((a0, a1, a2, a3)):
        maps[s] = a[...]
    totals = []
    for way in range(2):
        state = ident
        kept = ident
        for step in range(4):
            at = step if way == 0 else 3 - step
            kept = jnp.where(spot == at, state, kept)
            got = maps[(spot - at) & 3, way].astype(f32)
            state = got + ident if step == 0 else compose(state, got, row, lane)
        mine[way] = kept - ident
        totals.append(state)
    send[...] = jnp.where(level < 4, totals[0], totals[1]).astype(bf16)


def enter_body(scal, taken, mine, before, o0, o1, o2, o3, states):
    here, level = seat(scal, "sp_1"), seat(scal, "sp_0")
    row, lane = iota2((TOK, TOK))
    low = lane < 64
    other = jnp.where(low, taken[...].astype(f32), 0.0)
    enter = []
    for way in range(2):
        started = (level >= 4) if way == 0 else (level < 4)
        enter.append(compose(jnp.where(started, other, 0.0), mine[way], row, lane))
    for at in range(N_X):
        f, b = enter
        if at > 0:
            f = compose(f, before[at - 1, 0].astype(f32), row, lane)
        if at < N_X - 1:
            b = compose(b, before[N_X - 2 - at, 1].astype(f32), row, lane)
        states[at] = jnp.where(low, f, roll64(b)).astype(bf16)
    for s, out in enumerate((o0, o1, o2, o3)):
        out[...] = states[(here + s) & 3]


def final_body(
    scal, hgain, wa0, wp0, z0, z1, z2, z3, qeff, local, wa1, wp1, wa2, wp2, wa3, wp3, pool,
    keep, give, states, total,
):
    here, seq, core = seat(scal, "sp_1"), seat(scal, "fs"), seat(scal, "tp")
    row, lane = iota2((TOK, TOK))
    low = lane < 64
    top = row < 64
    for s, z in enumerate((z0, z1, z2, z3)):
        states[s] = z[...]
    cols = []
    for pair in range(PAIRS):
        c = slice(pair * 128, (pair + 1) * 128)
        packed = states[(here - pair) & 3].astype(f32)
        moved = roll64(packed)
        ahead = jnp.where(top, jnp.where(low, packed, 0.0), jnp.where(low, 0.0, moved))
        behind = jnp.where(top, jnp.where(low, moved, 0.0), jnp.where(low, 0.0, packed))
        block = jnp.concatenate([ahead, behind], axis=0).astype(bf16)
        read = dot(qeff[pair], block) + local[:, c]
        centred = read - head_sum(read) * (1.0 / 64.0)
        var = head_sum(centred * centred) * (1.0 / 64.0)
        cols.append(
            (centred * lax.rsqrt(var + head_eps) * hgain[:, c].astype(f32)).astype(bf16)
        )
    attn = jnp.concatenate(cols, axis=1)
    pooled = pool[...]
    weights = (
        (wa0[...], wp0[...]),
        (wa1[...], wp1[...]),
        (wa2[...], wp2[...]),
        (wa3[...], wp3[...]),
    )
    for s, (wa, wp) in enumerate(weights):
        at = pl.multiple_of(((seq - s) & 3) * 512, 512)
        total[:, pl.ds(at, 512)] = dot_t(attn, wa) + dot_t(pooled, wp)
    mine = pl.multiple_of(core * 64, 64)
    other = pl.multiple_of((1 - core) * 64, 64)
    keep[...] = total[pl.ds(mine, 64), :]
    give[...] = total[pl.ds(other, 64), :].astype(bf16)


def pool_body(scal, mix, pool_in, head, tail, out):
    core, span = seat(scal, "tp"), seat(scal, "sp_0") * N_X + seat(scal, "sp_1")
    here = pool_in[...].astype(f32)
    cells = jnp.concatenate([tail[...].astype(f32), here, head[...].astype(f32)], axis=0)
    spot = lax.broadcasted_iota(jnp.int32, (TOK, 256), 0) + span * TOK
    length = TOK * N_X * N_Z
    sums = []
    running = cells
    for level in range(4):
        shift = 2**level
        size = running.shape[0]
        running = running[: size - shift] + running[shift:]
        sums.append(running[REACH - shift : REACH - shift + TOK])
    for member in range(2):
        c = slice(member * 256, (member + 1) * 256)
        upper = core == 1
        chosen = jnp.where(upper, sums[member + 2][:, c], sums[member][:, c])
        half = jnp.where(upper, 2 ** (member + 2), 2**member)
        count = (jnp.minimum(spot + half, length) - jnp.maximum(spot - half, 0)).astype(f32)
        diff = (chosen / count - here[:, c]).astype(bf16)
        out[:, c] = dot(diff, mix[member]).astype(bf16)


def shift_by(a, axis, s, n):
    return lax.ppermute(a, axis, [(i, (i + s) % n) for i in range(n)])


def shards(
    inputs,
    input_norm_gain,
    receptance_matrix,
    key_matrix,
    value_matrix,
    pooling_input_weight,
    decay_lower_matrix,
    decay_raise_matrix,
    decay_offset_bias,
    removal_lower_matrix,
    removal_raise_matrix,
    removal_rate_bias,
    tempo_scale,
    sudden_decay_extra,
    head_norm_gain,
    group_mixing_weight,
    attention_output_matrix,
    pooling_output_matrix,
):
    scal = jnp.stack([lax.axis_index(a) for a in ("sp_1", "sp_0", "fs", "tp")]).astype(jnp.int32)
    return step(
        scal, inputs[0], input_norm_gain.reshape(1, 2048),
        receptance_matrix, key_matrix, value_matrix, pooling_input_weight,
        decay_lower_matrix, decay_raise_matrix.reshape(128, 512), decay_offset_bias,
        removal_lower_matrix, removal_raise_matrix.reshape(128, 512), removal_rate_bias,
        tempo_scale[0].reshape(16, TOK), sudden_decay_extra[0].reshape(16, TOK),
        head_norm_gain.reshape(1, 512), group_mixing_weight,
        attention_output_matrix, pooling_output_matrix,
    )


def step(
    scal, tokens, gain, wq, wk, wv, wp, dlow, draise, dbias, rlow, rraise, rbias,
    tempo, sudden, hgain, mix, attn_own, pool_own,
):
    rows = pl.pallas_call(
        cut_body,
        out_shape=[jax.ShapeDtypeStruct((TOK, 512), bf16)] * 4,
        in_specs=[pl.BlockSpec(memory_space=pltpu.SMEM), pl.BlockSpec(memory_space=pltpu.HBM)],
        out_specs=[pl.BlockSpec(memory_space=pltpu.VMEM)] * 4,
        scratch_shapes=[pltpu.SemaphoreType.DMA((4,))],
        compiler_params=pltpu.CompilerParams(vmem_limit_bytes=4 << 20),
        name="cut",
    )(scal, in_hbm(tokens))
    rows = list(rows)
    for s in (2, 1, 3):
        rows[s] = shift_by(rows[s], "fs", s, N_FS)
    square = (TOK, TOK)
    wk_near, wv_near, gain_near = stage(scal, wk, wv, gain)

    def give_back(got):
        back = [None] * 3
        for s in (2, 1, 3):
            back[s - 1] = shift_by(got[s - 1], "fs", N_FS - s, N_FS)
        return back

    parts = [((TOK, 1024), bf16)] * 3
    got = call(project_kv_body, parts)(
        scal, gain_near, wk_near, wv_near, *rows
    )
    kv = give_back(got)
    own_qp, *got = call(project_qp_body, [((TOK, 1024), f32)] + parts)(
        scal, gain_near, wq, wp, *rows
    )
    qp = [own_qp] + give_back(got)

    attn_w = [attn_own] + [None] * 3
    pool_w = [pool_own] + [None] * 3
    for s in (1, 3):
        attn_w[s] = shift_by(attn_own, "fs", s, N_FS)
        pool_w[s] = shift_by(pool_own, "fs", s, N_FS)
    attn_w[2] = shift_by(attn_w[1], "fs", 1, N_FS)
    pool_w[2] = shift_by(pool_w[3], "fs", 3, N_FS)

    inv, reach, factors = call(
        decay_body, [((TOK, 1), f32), ((2, TOK, 512), f32), ((8, 8, *square), bf16)], far=12
    )(
        scal, tokens, gain, dlow, rlow, draise, dbias, rraise, rbias, tempo, sudden, wk, wv, rows[0]
    )
    outs = call(
        maps_body,
        [((2, *square), bf16)] * 4 + [((8, N_BLK, *square), bf16), ((8, TOK, 256), bf16)],
        scratch=[pltpu.VMEM((16, *square), bf16)] * 3
        + [pltpu.VMEM((8, *square), bf16)] * 2
        + [pltpu.VMEM((PAIRS, *square), bf16), pltpu.VMEM((PAIRS, 2, *square), bf16)],
    )(scal, *kv, inv, factors, reach)
    maps, (right, xy) = outs[:4], outs[4:]
    got = [maps[0]]
    got += [shift_by(maps[s], "sp_1", s, N_X) for s in (1, 2, 3)]

    pool_sum = qp[0][:, 512:]
    for s in (1, 2, 3):
        pool_sum = pool_sum + qp[s][:, 512:].astype(f32)
    pool_in = (pool_sum * inv).astype(bf16)
    n_sp = N_X * N_Z
    below = lax.ppermute(pool_in[TOK - REACH :], SP, [(i, i + 1) for i in range(n_sp - 1)])
    above = lax.ppermute(pool_in[:REACH], SP, [(i + 1, i) for i in range(n_sp - 1)])

    (pooled,) = call(pool_body, [((TOK, 512), bf16)])(
        scal, mix, pool_in, above, below
    )
    qeff, local = call(
        read_body, [((PAIRS, TOK, 256), bf16), ((TOK, 512), f32)]
    )(scal, *qp, inv, right, reach, xy)

    total, before = call(
        chain_body,
        [((2, *square), bf16), ((3, 2, *square), bf16)],
        scratch=[pltpu.VMEM((N_X, 2, *square), bf16)],
    )(scal, *got)
    near = [total]
    for s in (1, 2, 3):
        pairs = [(i, (i // 4) * 4 + (i + s) % 4) for i in range(N_Z)]
        near.append(lax.ppermute(total, "sp_0", pairs))
    half, mine = call(
        group_body,
        [(square, bf16), ((2, *square), f32)],
        scratch=[pltpu.VMEM((4, 2, *square), bf16)],
    )(scal, *near)
    taken = lax.ppermute(half, "sp_0", [(i, i ^ 4) for i in range(N_Z)])
    states = call(
        enter_body, [(square, bf16)] * 4, scratch=[pltpu.VMEM((N_X, *square), bf16)]
    )(scal, taken, mine, before)
    enter = [states[0]]
    enter += [shift_by(states[s], "sp_1", s, N_X) for s in (1, 2, 3)]

    keep, give = call(
        final_body,
        [((64, 2048), f32), ((64, 2048), bf16)],
        scratch=[pltpu.VMEM((N_X, *square), bf16), pltpu.VMEM((TOK, 2048), f32)],
    )(
        scal, hgain, attn_own, pool_own, *enter, qeff, local,
        attn_w[1], pool_w[1], attn_w[2], pool_w[2], attn_w[3], pool_w[3], pooled,
    )
    taken = lax.ppermute(give, "tp", [(0, 1), (1, 0)])
    return (keep + taken.astype(f32)).astype(bf16)[None]


def solution(mesh):
    split = Mesh(
        mesh.devices.reshape(8, 4, mesh.shape["fs"], mesh.shape["tp"]), ("sp_0", "sp_1", "fs", "tp")
    )
    in_specs = (
        P("fs", SP, None),
        P(),
        P("fs", "tp"),
        P("fs", "tp"),
        P("fs", "tp"),
        P("fs", "tp"),
        P(),
        P(None, None, "tp"),
        P(None, "tp"),
        P(),
        P(None, None, "tp"),
        P(None, "tp"),
        P("fs", None, "tp", SP),
        P("fs", None, "tp", SP),
        P("tp"),
        P("tp", None, None),
        P("fs", "tp"),
        P("fs", "tp"),
    )
    out_specs = P("fs", SP_TP, None)
    return jax.shard_map(
        shards, mesh=split, in_specs=in_specs, out_specs=out_specs, check_vma=False
    )
```

```python
import jax
import jax.numpy as jnp
from jax import lax
from jax.experimental import pallas as pl
from jax.experimental.pallas import tpu as pltpu
from jax.sharding import Mesh
from jax.sharding import PartitionSpec as P

SP = ("sp_0", "sp_1")
SP_TP = ("sp_0", "sp_1", "tp")
N_FS, N_X, N_Z = 4, 4, 8
TOK = 128
BLK = 32
N_BLK = TOK // BLK
PAIRS = 4
REACH = 8
LEFT, LEAD, TAIL, OWN = 4, 5, 6, 7

norm_eps = 1e-06
head_eps = 0.00064
unit_eps = 1e-06
half_root = 0.6065306597126334
cap = 80.0

f32 = jnp.float32
bf16 = jnp.bfloat16
highest = lax.Precision.HIGHEST


def in_hbm(array):
    return pltpu.with_memory_space_constraint(array, pltpu.HBM)


def call(body, outs, scratch=(), far=0, keep=0):
    def run(scal, *arrays):
        count = len(arrays) - far + len(outs)

        def fetched(at, *refs):
            source, near, held = refs[:far], refs[far : far + count], refs[far + count :]
            kept = near[count - keep :]
            buffers, sems, rest = held[: far - keep], held[far - keep], held[far - keep + 1 :]
            buffers = (*kept, *buffers)
            copies = [
                pltpu.make_async_copy(a, b, sems.at[k])
                for k, (a, b) in enumerate(zip(source, buffers))
            ]
            for copy in copies:
                copy.start()
            for copy in copies:
                copy.wait()
            body(at, *buffers, *near[: count - keep], *rest)

        extra = []
        if far:
            extra = [pltpu.VMEM(a.shape, a.dtype) for a in arrays[keep:far]]
            extra.append(pltpu.SemaphoreType.DMA((far,)))
        return pl.pallas_call(
            fetched if far else body,
            out_shape=[jax.ShapeDtypeStruct(s, d) for s, d in outs],
            in_specs=[pl.BlockSpec(memory_space=pltpu.SMEM)]
            + [pl.BlockSpec(memory_space=pltpu.HBM)] * far
            + [pl.BlockSpec(memory_space=pltpu.VMEM)] * (len(arrays) - far),
            out_specs=[pl.BlockSpec(memory_space=pltpu.VMEM)] * len(outs),
            scratch_shapes=extra + list(scratch),
            compiler_params=pltpu.CompilerParams(vmem_limit_bytes=20 << 20),
            cost_estimate=pl.CostEstimate(flops=1, transcendentals=0, bytes_accessed=1),
        )(scal, *[in_hbm(a) for a in arrays[:far]], *arrays[far:])

    return run


def seat(scal, axis):
    return scal[("sp_1", "sp_0", "fs", "tp").index(axis)]


def cut_body(scal, tokens, *refs):
    outs, sems = refs[:4], refs[4]
    copies = []
    for s, out in enumerate(outs):
        at = pl.multiple_of(((seat(scal, "fs") + s) & 3) * 512, 512)
        copies.append(pltpu.make_async_copy(tokens.at[:, pl.ds(at, 512)], out, sems.at[s]))
        copies[-1].start()
    for copy in copies:
        copy.wait()


def dot(a, b):
    return jnp.dot(a, b, preferred_element_type=f32)


def dot_t(a, b):
    return lax.dot_general(a, b, (((1,), (1,)), ((), ())), preferred_element_type=f32)


def dot_0(a, b):
    return lax.dot_general(a, b, (((0,), (0,)), ((), ())), preferred_element_type=f32)


def iota2(shape):
    return (
        lax.broadcasted_iota(jnp.int32, shape, 0),
        lax.broadcasted_iota(jnp.int32, shape, 1),
    )


def roll64(a):
    return pltpu.roll(a, 64, axis=1)


def summed(own, parts, cols, scale):
    r1, r2, r3 = parts
    got = own + r1[:, cols].astype(f32)
    got = got + r2[:, cols].astype(f32) + r3[:, cols].astype(f32)
    return (got * scale).astype(bf16).astype(f32)


def head_sum(a):
    row, lane = iota2((128, 128))
    same = jnp.where((row // 64) == (lane // 64), 1.0, 0.0).astype(f32)
    return jnp.dot(a, same, precision=highest, preferred_element_type=f32)


def mid_rows(way):
    return [i * BLK + (BLK // 2 - 1 if way == 0 else BLK // 2) for i in range(N_BLK)]


def both_heads(block, lane):
    zero = jnp.zeros_like(block)
    low = lane < 64
    return jnp.concatenate(
        [jnp.where(low, block, zero), jnp.where(low, zero, block)], axis=0
    ).astype(bf16)


def gather_rows(scal, gain, parts):
    at = pl.multiple_of(seat(scal, "fs") * 512, 512)
    rows = jnp.concatenate([part[...] for part in parts], axis=0).astype(f32)
    return (rows * gain[:, pl.ds(at, 512)].astype(f32)).astype(bf16)


def put_parts(got, outs, cols):
    for s in (1, 2, 3):
        outs[s - 1][:, cols] = got[s * TOK : (s + 1) * TOK].astype(bf16)


def project_qp_body(scal, gain, w1, w2, a0, a1, a2, a3, own, *outs):
    rows = gather_rows(scal, gain, (a0, a1, a2, a3))
    for half, w in enumerate((w1, w2)):
        cols = slice(half * 512, (half + 1) * 512)
        got = dot(rows, w[...])
        own[:, cols] = got[:TOK]
        put_parts(got, outs, cols)


def project_kv_body(scal, gain, w1, w2, a0, a1, a2, a3, *outs):
    rows = gather_rows(scal, gain, (a0, a1, a2, a3))
    for half, w in enumerate((w1, w2)):
        put_parts(dot(rows, w[...]), outs, slice(half * 512, (half + 1) * 512))


def decay_body(
    scal,
    wk, wv, gain, tokens, dlow, rlow, draise, rraise, tempo_in, sudden_in, dbias, rbias, mine,
    inv_out, reach_out, out,
):
    rows = gather_rows(scal, gain, (mine,))
    for half, w in enumerate((wk, wv)):
        got = dot(rows, w[...])
        for pair in range(PAIRS):
            out[half * PAIRS + pair, OWN] = got[:, pair * 128 : (pair + 1) * 128].astype(bf16)
    row, lane = iota2((TOK, TOK))
    low = lane < 64
    tempo = tempo_in[...].T
    sudden = sudden_in[...].T
    wide = tokens[...].astype(f32)
    inv = lax.rsqrt(jnp.mean(wide * wide, axis=-1, keepdims=True) + norm_eps)
    inv_out[...] = inv
    normed = (wide * inv * gain[:, :2048].astype(f32)).astype(bf16)
    act = jnp.tanh(dot(normed, dlow[...]).astype(bf16).astype(f32)).astype(bf16)
    lat = dot(normed, rlow[...]).astype(bf16)
    for way in range(2):
        mine = (lane // 64) == way
        act_w = jnp.where(mine, act, jnp.zeros_like(act))
        lat_w = jnp.where(mine, lat, jnp.zeros_like(lat))
        tri = jnp.where((row >= lane) if way == 0 else (row <= lane), 1.0, 0.0).astype(f32)
        for pair in range(PAIRS):
            cols = slice(pair * 128, (pair + 1) * 128)
            chain = way * PAIRS + pair
            pre = dbias[way : way + 1, cols] + dot(act_w, draise[:, cols])
            rate = jax.nn.sigmoid(rbias[way : way + 1, cols] + dot(lat_w, rraise[:, cols]))
            at = way * 8 + pair * 2
            pace = jnp.where(low, tempo[:, at : at + 1], tempo[:, at + 1 : at + 2])
            jump = jnp.where(low, sudden[:, at : at + 1], sudden[:, at + 1 : at + 2])
            g = -half_root * jax.nn.sigmoid(pre) * pace + jump
            reach = jnp.dot(tri, g, precision=highest, preferred_element_type=f32)
            reach_out[way, :, cols] = reach
            before = reach - g
            out[chain, LEAD] = jnp.exp(before).astype(bf16)
            for i, mid_row in enumerate(mid_rows(way)):
                mid = reach[mid_row : mid_row + 1, :]
                rows = slice(i * BLK, (i + 1) * BLK)
                out[chain, LEFT, rows] = jnp.exp(before[rows] - mid).astype(bf16)
                out[chain, i] = (rate * jnp.exp(jnp.minimum(mid - reach, cap))).astype(bf16)
            end = reach[TOK - 1 :, :] if way == 0 else reach[:1, :]
            out[chain, TAIL] = (rate * jnp.exp(end - reach)).astype(bf16)


def maps_body(
    scal,
    r1, r2, r3, inv, factors, reach,
    o0, o1, o2, o3, right_out, xy_out, solved, links, inner, ahead_out, tail_out, strong_out, maps,
):
    here = seat(scal, "sp_1")
    row, lane = iota2((TOK, TOK))
    low = lane < 64
    wide_low = (lax.broadcasted_iota(jnp.int32, (TOK, 256), 1) % 128) < 64
    eye = row == lane
    eye_bf = jnp.where(row == lane, 1.0, 0.0).astype(bf16)
    level_masks = []
    for level in range(7):
        size = 2**level
        hit = ((row // (2 * size)) == (lane // (2 * size))) & ((row // size) != (lane // size))
        level_masks.append(jnp.where(hit, 1.0, 0.0).astype(bf16))
    scale = inv[...]
    for pair in range(PAIRS):
        c = slice(pair * 128, (pair + 1) * 128)
        v = slice(512 + pair * 128, 512 + (pair + 1) * 128)
        key = summed(factors[pair, OWN].astype(f32), (r1, r2, r3), c, scale)
        square = head_sum(key * key) + unit_eps
        inverse = lax.rsqrt(square)
        unit = key * inverse
        val = summed(factors[PAIRS + pair, OWN].astype(f32), (r1, r2, r3), v, scale)
        strong_out[pair] = (val * (square * inverse)).astype(bf16)
        for way in range(2):
            chain = way * PAIRS + pair
            pieces = []
            for i in range(N_BLK):
                rows = slice(i * BLK, (i + 1) * BLK)
                side = (unit * factors[chain, i].astype(f32)).astype(bf16)
                right_out[chain, i] = side
                pieces.append(
                    dot_t(both_heads(unit[rows] * factors[chain, LEFT, rows].astype(f32), lane[:BLK]), side)
                )
            strict = (row > lane) if way == 0 else (row < lane)
            for head in range(2):
                link = jnp.concatenate(
                    [piece[head * BLK : (head + 1) * BLK] for piece in pieces], axis=0
                )
                link = jnp.where(strict, link, 0.0).astype(bf16)
                links[2 * chain + head] = link
                solved[2 * chain + head] = eye_bf - link * level_masks[0]
            ahead_out[chain] = (unit * factors[chain, LEAD].astype(f32)).astype(bf16)
            tail_out[chain] = (unit * factors[chain, TAIL].astype(f32)).astype(bf16)
    for level in range(1, 7):
        for k in range(16):
            inner[k] = dot(links[k] * level_masks[level], solved[k]).astype(bf16)
        for k in range(16):
            solved[k] = solved[k] - dot(solved[k], inner[k]).astype(bf16)
    for pair in range(PAIRS):
        c = slice(pair * 128, (pair + 1) * 128)
        for way in range(2):
            chain = way * PAIRS + pair
            side = jnp.concatenate([strong_out[pair], ahead_out[chain]], axis=1)
            first = dot(solved[2 * chain], side)
            second = dot(solved[2 * chain + 1], side)
            xy = jnp.where(wide_low, first, second).astype(bf16)
            xy_out[chain] = xy
            got = dot_0(tail_out[chain], xy)
            carry = got[:, :128]
            end = reach[way, TOK - 1 :, c] if way == 0 else reach[way, :1, c]
            turn = jnp.where(eye, jnp.exp(end) - 1.0, 0.0) - got[:, 128:]
            maps[pair, way] = jnp.where(
                row < 64,
                jnp.where(low, carry, roll64(turn)),
                jnp.where(low, roll64(carry), turn),
            ).astype(bf16)
    for s, out in enumerate((o0, o1, o2, o3)):
        out[...] = maps[(here + s) & 3]


def read_body(scal, own, r1, r2, r3, inv, right, reach_in, xy_in, qeff, local, pool, first, last):
    row, lane = iota2((TOK, TOK))
    wide_low = (lax.broadcasted_iota(jnp.int32, (TOK, 256), 1) % 128) < 64
    scale = inv[...]
    for pair in range(PAIRS):
        c = slice(pair * 128, (pair + 1) * 128)
        query = summed(own[:, c], (r1, r2, r3), c, scale)
        base = None
        for way in range(2):
            reach = reach_in[way, :, c]
            pieces = []
            for i, mid_row in enumerate(mid_rows(way)):
                mid = reach[mid_row : mid_row + 1, :]
                rows = slice(i * BLK, (i + 1) * BLK)
                left = query[rows] * jnp.exp(reach[rows] - mid)
                pieces.append(
                    dot_t(both_heads(left, lane[:BLK]), right[way * PAIRS + pair, i])
                )
            within = (row >= lane) if way == 0 else (row <= lane)
            xy = xy_in[way * PAIRS + pair]
            pulls = []
            for head in range(2):
                link = jnp.concatenate(
                    [piece[head * BLK : (head + 1) * BLK] for piece in pieces], axis=0
                )
                pulls.append(dot(jnp.where(within, link, 0.0).astype(bf16), xy))
            pull = jnp.where(wide_low, pulls[0], pulls[1])
            base = pull[:, :128] if base is None else base + pull[:, :128]
            qeff[pair, :, way * 128 : (way + 1) * 128] = (
                query * jnp.exp(reach) - pull[:, 128:]
            ).astype(bf16)
        local[:, c] = base
        v = slice(512 + pair * 128, 512 + (pair + 1) * 128)
        value = summed(own[:, v], (r1, r2, r3), v, scale)
        pool[:, c] = value.astype(bf16)
        first[:, c] = value[:REACH].astype(bf16)
        last[:, c] = value[TOK - REACH :].astype(bf16)


def spread(packed, row, lane):
    moved = roll64(packed)
    return jnp.where(
        row < 64,
        jnp.where(lane < 64, moved, 0.0),
        jnp.where(lane < 64, 0.0, packed),
    ).astype(bf16)


def compose(state, packed, row, lane):
    return (
        state
        + dot(spread(packed, row, lane), state.astype(bf16))
        + jnp.where(lane < 64, packed, 0.0)
    )


def chain_body(scal, a0, a1, a2, a3, send, before, maps):
    here = seat(scal, "sp_1")
    row, lane = iota2((TOK, TOK))
    ident = jnp.where((lane - 64) == (row % 64), 1.0, 0.0).astype(f32)
    for s, a in enumerate((a0, a1, a2, a3)):
        maps[s] = a[...]
    for way in range(2):
        state = ident
        for step in range(N_X):
            at = step if way == 0 else N_X - 1 - step
            got = maps[(here - at) & 3, way].astype(f32)
            state = got + ident if step == 0 else compose(state, got, row, lane)
            if step < N_X - 1:
                before[step, way] = (state - ident).astype(bf16)
        send[way] = (state - ident).astype(bf16)


def group_body(scal, a0, a1, a2, a3, send, mine, maps):
    level = seat(scal, "sp_0")
    spot = level & 3
    row, lane = iota2((TOK, TOK))
    ident = jnp.where((lane - 64) == (row % 64), 1.0, 0.0).astype(f32)
    for s, a in enumerate((a0, a1, a2, a3)):
        maps[s] = a[...]
    totals = []
    for way in range(2):
        state = ident
        kept = ident
        for step in range(4):
            at = step if way == 0 else 3 - step
            kept = jnp.where(spot == at, state, kept)
            got = maps[(spot - at) & 3, way].astype(f32)
            state = got + ident if step == 0 else compose(state, got, row, lane)
        mine[way] = kept - ident
        totals.append(state)
    send[...] = jnp.where(level < 4, totals[0], totals[1]).astype(bf16)


def enter_body(scal, taken, mine, before, o0, o1, o2, o3, states):
    here, level = seat(scal, "sp_1"), seat(scal, "sp_0")
    row, lane = iota2((TOK, TOK))
    low = lane < 64
    other = jnp.where(low, taken[...].astype(f32), 0.0)
    enter = []
    for way in range(2):
        started = (level >= 4) if way == 0 else (level < 4)
        enter.append(compose(jnp.where(started, other, 0.0), mine[way], row, lane))
    for at in range(N_X):
        f, b = enter
        if at > 0:
            f = compose(f, before[at - 1, 0].astype(f32), row, lane)
        if at < N_X - 1:
            b = compose(b, before[N_X - 2 - at, 1].astype(f32), row, lane)
        states[at] = jnp.where(low, f, roll64(b)).astype(bf16)
    for s, out in enumerate((o0, o1, o2, o3)):
        out[...] = states[(here + s) & 3]


def final_body(
    scal, gain, wa0, wp0, z0, z1, z2, z3, qeff, local, wa1, wp1, wa2, wp2, wa3, wp3, pool,
    keep, give, states, total,
):
    here, seq, core = seat(scal, "sp_1"), seat(scal, "fs"), seat(scal, "tp")
    row, lane = iota2((TOK, TOK))
    low = lane < 64
    top = row < 64
    for s, z in enumerate((z0, z1, z2, z3)):
        states[s] = z[...]
    cols = []
    for pair in range(PAIRS):
        c = slice(pair * 128, (pair + 1) * 128)
        at = slice(2048 + pair * 128, 2048 + (pair + 1) * 128)
        packed = states[(here - pair) & 3].astype(f32)
        moved = roll64(packed)
        ahead = jnp.where(top, jnp.where(low, packed, 0.0), jnp.where(low, 0.0, moved))
        behind = jnp.where(top, jnp.where(low, moved, 0.0), jnp.where(low, 0.0, packed))
        block = jnp.concatenate([ahead, behind], axis=0).astype(bf16)
        read = dot(qeff[pair], block) + local[:, c]
        centred = read - head_sum(read) * (1.0 / 64.0)
        var = head_sum(centred * centred) * (1.0 / 64.0)
        cols.append(
            (centred * lax.rsqrt(var + head_eps) * gain[:, at].astype(f32)).astype(bf16)
        )
    attn = jnp.concatenate(cols, axis=1)
    pooled = pool[...]
    weights = (
        (wa0[...], wp0[...]),
        (wa1[...], wp1[...]),
        (wa2[...], wp2[...]),
        (wa3[...], wp3[...]),
    )
    for s, (wa, wp) in enumerate(weights):
        at = pl.multiple_of(((seq - s) & 3) * 512, 512)
        total[:, pl.ds(at, 512)] = dot_t(attn, wa) + dot_t(pooled, wp)
    mine = pl.multiple_of(core * 64, 64)
    other = pl.multiple_of((1 - core) * 64, 64)
    keep[...] = total[pl.ds(mine, 64), :]
    give[...] = total[pl.ds(other, 64), :].astype(bf16)


def pool_body(scal, mix, pool_in, head, tail, out):
    core, span = seat(scal, "tp"), seat(scal, "sp_0") * N_X + seat(scal, "sp_1")
    here = pool_in[...].astype(f32)
    cells = jnp.concatenate([tail[...].astype(f32), here, head[...].astype(f32)], axis=0)
    spot = lax.broadcasted_iota(jnp.int32, (TOK, 256), 0) + span * TOK
    length = TOK * N_X * N_Z
    sums = []
    running = cells
    for level in range(4):
        shift = 2**level
        size = running.shape[0]
        running = running[: size - shift] + running[shift:]
        sums.append(running[REACH - shift : REACH - shift + TOK])
    for member in range(2):
        c = slice(member * 256, (member + 1) * 256)
        upper = core == 1
        chosen = jnp.where(upper, sums[member + 2][:, c], sums[member][:, c])
        half = jnp.where(upper, 2 ** (member + 2), 2**member)
        count = (jnp.minimum(spot + half, length) - jnp.maximum(spot - half, 0)).astype(f32)
        diff = (chosen / count - here[:, c]).astype(bf16)
        out[:, c] = dot(diff, mix[member]).astype(bf16)


def shift_by(a, axis, s, n):
    return lax.ppermute(a, axis, [(i, (i + s) % n) for i in range(n)])


def shards(
    inputs,
    input_norm_gain,
    receptance_matrix,
    key_matrix,
    value_matrix,
    pooling_input_weight,
    decay_lower_matrix,
    decay_raise_matrix,
    decay_offset_bias,
    removal_lower_matrix,
    removal_raise_matrix,
    removal_rate_bias,
    tempo_scale,
    sudden_decay_extra,
    head_norm_gain,
    group_mixing_weight,
    attention_output_matrix,
    pooling_output_matrix,
):
    scal = jnp.stack([lax.axis_index(a) for a in ("sp_1", "sp_0", "fs", "tp")]).astype(jnp.int32)
    return step(
        scal, inputs[0],
        jnp.concatenate([input_norm_gain, head_norm_gain]).reshape(1, 2560),
        receptance_matrix, key_matrix, value_matrix, pooling_input_weight,
        decay_lower_matrix, decay_raise_matrix.reshape(128, 512), decay_offset_bias,
        removal_lower_matrix, removal_raise_matrix.reshape(128, 512), removal_rate_bias,
        tempo_scale[0].reshape(16, TOK), sudden_decay_extra[0].reshape(16, TOK),
        group_mixing_weight,
        attention_output_matrix, pooling_output_matrix,
    )


def step(
    scal, tokens, gain, wq, wk, wv, wp, dlow, draise, dbias, rlow, rraise, rbias,
    tempo, sudden, mix, attn_own, pool_own,
):
    rows = pl.pallas_call(
        cut_body,
        out_shape=[jax.ShapeDtypeStruct((TOK, 512), bf16)] * 4,
        in_specs=[pl.BlockSpec(memory_space=pltpu.SMEM), pl.BlockSpec(memory_space=pltpu.HBM)],
        out_specs=[pl.BlockSpec(memory_space=pltpu.VMEM)] * 4,
        scratch_shapes=[pltpu.SemaphoreType.DMA((4,))],
        compiler_params=pltpu.CompilerParams(vmem_limit_bytes=4 << 20),
        name="cut",
    )(scal, in_hbm(tokens))
    rows = list(rows)
    for s in (2, 1, 3):
        rows[s] = shift_by(rows[s], "fs", s, N_FS)
    square = (TOK, TOK)
    inv, reach, factors, wk_near, wv_near, gain_near = call(
        decay_body,
        [
            ((TOK, 1), f32), ((2, TOK, 512), f32), ((8, 8, *square), bf16),
            (wk.shape, bf16), (wv.shape, bf16), (gain.shape, bf16),
        ],
        far=12,
        keep=3,
    )(
        scal, wk, wv, gain, tokens, dlow, rlow, draise, rraise, tempo, sudden, dbias, rbias, rows[0]
    )

    def give_back(got):
        back = [None] * 3
        for s in (2, 1, 3):
            back[s - 1] = shift_by(got[s - 1], "fs", N_FS - s, N_FS)
        return back

    parts = [((TOK, 1024), bf16)] * 3
    got = call(project_kv_body, parts)(
        scal, gain_near, wk_near, wv_near, *rows
    )
    kv = give_back(got)
    own_qp, *got = call(project_qp_body, [((TOK, 1024), f32)] + parts)(
        scal, gain_near, wq, wp, *rows
    )
    qp = [own_qp] + give_back(got)

    attn_w = [attn_own] + [None] * 3
    pool_w = [pool_own] + [None] * 3
    attn_w[1] = shift_by(attn_own, "fs", 1, N_FS)
    pool_w[3] = shift_by(pool_own, "fs", 3, N_FS)
    attn_w[3] = shift_by(attn_own, "fs", 3, N_FS)
    pool_w[1] = shift_by(pool_own, "fs", 1, N_FS)
    attn_w[2] = shift_by(attn_w[1], "fs", 1, N_FS)
    pool_w[2] = shift_by(pool_w[3], "fs", 3, N_FS)

    outs = call(
        maps_body,
        [((2, *square), bf16)] * 4 + [((8, N_BLK, *square), bf16), ((8, TOK, 256), bf16)],
        scratch=[pltpu.VMEM((16, *square), bf16)] * 3
        + [pltpu.VMEM((8, *square), bf16)] * 2
        + [pltpu.VMEM((PAIRS, *square), bf16), pltpu.VMEM((PAIRS, 2, *square), bf16)],
    )(scal, *kv, inv, factors, reach)
    maps, (right, xy) = outs[:4], outs[4:]
    got = [maps[0]]
    got += [shift_by(maps[s], "sp_1", s, N_X) for s in (1, 2, 3)]

    qeff, local, pool_in, first, last = call(
        read_body,
        [
            ((PAIRS, TOK, 256), bf16), ((TOK, 512), f32),
            ((TOK, 512), bf16), ((REACH, 512), bf16), ((REACH, 512), bf16),
        ],
    )(scal, *qp, inv, right, reach, xy)
    n_sp = N_X * N_Z
    below = lax.ppermute(last, SP, [(i, i + 1) for i in range(n_sp - 1)])
    above = lax.ppermute(first, SP, [(i + 1, i) for i in range(n_sp - 1)])
    (pooled,) = call(pool_body, [((TOK, 512), bf16)])(
        scal, mix, pool_in, above, below
    )
    total, before = call(
        chain_body,
        [((2, *square), bf16), ((3, 2, *square), bf16)],
        scratch=[pltpu.VMEM((N_X, 2, *square), bf16)],
    )(scal, *got)
    near = [total]
    for s in (1, 2, 3):
        pairs = [(i, (i // 4) * 4 + (i + s) % 4) for i in range(N_Z)]
        near.append(lax.ppermute(total, "sp_0", pairs))
    half, mine = call(
        group_body,
        [(square, bf16), ((2, *square), f32)],
        scratch=[pltpu.VMEM((4, 2, *square), bf16)],
    )(scal, *near)
    taken = lax.ppermute(half, "sp_0", [(i, i ^ 4) for i in range(N_Z)])
    states = call(
        enter_body, [(square, bf16)] * 4, scratch=[pltpu.VMEM((N_X, *square), bf16)]
    )(scal, taken, mine, before)
    enter = [states[0]]
    enter += [shift_by(states[s], "sp_1", s, N_X) for s in (1, 2, 3)]

    keep, give = call(
        final_body,
        [((64, 2048), f32), ((64, 2048), bf16)],
        scratch=[pltpu.VMEM((N_X, *square), bf16), pltpu.VMEM((TOK, 2048), f32)],
    )(
        scal, gain_near, attn_own, pool_own, *enter, qeff, local,
        attn_w[1], pool_w[1], attn_w[2], pool_w[2], attn_w[3], pool_w[3], pooled,
    )
    taken = lax.ppermute(give, "tp", [(0, 1), (1, 0)])
    return (keep + taken.astype(f32)).astype(bf16)[None]


def solution(mesh):
    split = Mesh(
        mesh.devices.reshape(8, 4, mesh.shape["fs"], mesh.shape["tp"]), ("sp_0", "sp_1", "fs", "tp")
    )
    in_specs = (
        P("fs", SP, None),
        P(),
        P("fs", "tp"),
        P("fs", "tp"),
        P("fs", "tp"),
        P("fs", "tp"),
        P(),
        P(None, None, "tp"),
        P(None, "tp"),
        P(),
        P(None, None, "tp"),
        P(None, "tp"),
        P("fs", None, "tp", SP),
        P("fs", None, "tp", SP),
        P("tp"),
        P("tp", None, None),
        P("fs", "tp"),
        P("fs", "tp"),
    )
    out_specs = P("fs", SP_TP, None)
    return jax.shard_map(
        shards, mesh=split, in_specs=in_specs, out_specs=out_specs, check_vma=False
    )
```
